32 devices in a mesh: rep: 2 (over x), fs: 8 (over z, y), tp: 2 (over core).
Axes of the slice: x: 2, y: 2, z: 4, core: 2. Of those that a mesh axis runs over, the one named last changes fastest.
Arguments:
- inputs: bfloat16 [8192, 2048], P(('rep', 'fs')), may hold values from -6 to 6
- cotangent: bfloat16 [8192, 2048], P(('rep', 'fs')), may hold values from -6 to 6
- gate_pre: bfloat16 [8192, 5632], P(('rep', 'fs'), 'tp'), may hold values from -8 to 8
- up_pre: bfloat16 [8192, 5632], P(('rep', 'fs'), 'tp'), may hold values from -6 to 6
- gate_weight: float32 [2048, 5632], P('fs', 'tp'), may hold values from -0.125 to 0.125
- up_weight: float32 [2048, 5632], P('fs', 'tp'), may hold values from -0.125 to 0.125
- down_weight: float32 [2048, 5632], P('fs', 'tp'), may hold values from -0.078125 to 0.078125
- gate_scale: float32 [1, 5632], P(None, 'tp'), may hold values from 0.1 to 1.9
- up_scale: float32 [1, 5632], P(None, 'tp'), may hold values from 0.1 to 1.9
- down_scale: float32 [1, 5632], P(None, 'tp'), may hold values from 0.1 to 1.9
Outputs:
- input_grad: bfloat16 [8192, 2048], P(('rep', 'fs'), 'tp')
- gate_grad: float32 [2048, 5632], P('fs', 'tp')
- up_grad: float32 [2048, 5632], P('fs', 'tp')
- down_grad: float32 [2048, 5632], P('fs', 'tp')
The draws below stay inside these ranges and needn't reach their ends.
All inputs are finite; a program needn't handle non-finite values.
Results may differ from the reference program's by a relative error of at most 0.018.
Values may be sent and summed in bfloat16 or wider, within the bound.
No kernel may reach another device: no remote copies, remote signals or barrier semaphores. Data moves between devices by JAX's collectives and lax.ppermute only.
A program may use at most 192 MiB of HBM per device.

```python
import jax
import jax.numpy as jnp
from jax import lax

D = 2048
FF = 5632
TOKENS = 8192
N_TP = 2


def spiked(array, own_key, source, target, blocks, factor):
    owner, partner = [(jnp.arange(array.shape[position]) // (array.shape[position] // blocks)).reshape([-1 if axis == position else 1 for axis in range(array.ndim)]) for position in (source, target)]
    chosen = jax.random.permutation(own_key, blocks)[partner]
    strong = (owner == chosen) | (owner == (partner + blocks // 2) % blocks)
    return jnp.where(strong, factor * array, array)


def level_of(key, extent, shards, least, top_value):
    factor_of, own = 1.0, jax.random.fold_in(key, 6)
    for axis_at, parts in shards:
        draws = jnp.exp(jax.random.uniform(jax.random.fold_in(own, axis_at), (parts,), jnp.float32, least / len(shards), top_value / len(shards)))
        factor_of = factor_of * jnp.repeat(draws, extent[axis_at] // parts).reshape([-1 if axis == axis_at else 1 for axis in range(len(extent))])
    return factor_of


def normal_values(own_key, extent, scale, reach, shards=(), kind=jnp.bfloat16):
    level = level_of(own_key, extent, shards, -0.22, 0.18) if shards else 1.0
    entries = jax.random.normal(own_key, extent, jnp.float32) * scale * level
    return jnp.minimum(jnp.maximum(entries, -reach), reach).astype(kind)


def heavy_noise(own_key, extent, deviation, reach, pieces, heavy, kind=jnp.bfloat16):
    result = deviation * jax.random.normal(own_key, extent, jnp.float32)
    if pieces:
        result = result * level_of(own_key, extent, pieces, -0.22, 0.18)
    return jnp.clip(spiked(result, jax.random.fold_in(own_key, 3), *heavy), -reach, reach).astype(kind)


def setup_inputs(seed: int = 0) -> dict:
    arg_keys = jax.random.split(jax.random.key(seed), 11)
    inputs = normal_values(arg_keys[0], (TOKENS, D), 1.0, 6.0, ((0, 16),))
    cotangent = heavy_noise(arg_keys[1], (TOKENS, D), 1.0, 6.0, ((0, 16),), (0, 1, 16, 2.0))
    gate_pre = normal_values(arg_keys[2], (TOKENS, FF), 1.5, 8.0, ((0, 16), (1, 2)))
    up_pre = normal_values(arg_keys[3], (TOKENS, FF), 1.0, 6.0, ((0, 16), (1, 2)))
    gate_weight = normal_values(arg_keys[4], (D, FF), D ** -0.5, 0.125, ((0, 8), (1, 2)), jnp.float32)
    up_weight = normal_values(arg_keys[5], (D, FF), D ** -0.5, 0.125, ((0, 8), (1, 2)), jnp.float32)
    down_weight = normal_values(arg_keys[6], (D, FF), FF ** -0.5, 0.078125, ((0, 8), (1, 2)), jnp.float32)
    gate_scale = jnp.clip(1.0 + 0.18 * jax.random.normal(arg_keys[7], (1, FF), jnp.float32), 0.1, 1.9)
    up_scale = jnp.clip(1.0 + 0.18 * jax.random.normal(arg_keys[8], (1, FF), jnp.float32), 0.1, 1.9)
    down_scale = jnp.clip(1.0 + 0.18 * jax.random.normal(arg_keys[9], (1, FF), jnp.float32), 0.1, 1.9)
    return dict(inputs=inputs, cotangent=cotangent, gate_pre=gate_pre, up_pre=up_pre, gate_weight=gate_weight, up_weight=up_weight, down_weight=down_weight, gate_scale=gate_scale, up_scale=up_scale, down_scale=down_scale)


def reference(inputs, cotangent, gate_pre, up_pre, gate_weight, up_weight, down_weight, gate_scale, up_scale, down_scale):
    gate = gate_pre.astype(jnp.float32)
    upper = up_pre.astype(jnp.float32)
    sig = jax.nn.sigmoid(gate)
    act = gate * sig
    hidden = (act * upper).astype(jnp.bfloat16)
    down_bf = down_weight.astype(jnp.bfloat16)
    hidden_cot = jnp.dot(cotangent, down_bf, preferred_element_type=jnp.float32) * down_scale
    gate_cot = (hidden_cot * upper * sig * (1.0 + gate * (1.0 - sig)) * gate_scale).astype(jnp.bfloat16)
    up_cot = (hidden_cot * act * up_scale).astype(jnp.bfloat16)
    width = FF // N_TP
    gate_bf = gate_weight.astype(jnp.bfloat16)
    up_bf = up_weight.astype(jnp.bfloat16)

    def block_sum(total, index):
        start = (index * width).astype(jnp.int32)
        gc = lax.dynamic_slice_in_dim(gate_cot, start, width, 1)
        uc = lax.dynamic_slice_in_dim(up_cot, start, width, 1)
        gw = lax.dynamic_slice_in_dim(gate_bf, start, width, 1)
        uw = lax.dynamic_slice_in_dim(up_bf, start, width, 1)
        part = jnp.dot(gc, gw.T, preferred_element_type=jnp.float32) + jnp.dot(uc, uw.T, preferred_element_type=jnp.float32)
        return total + part.astype(jnp.bfloat16).astype(jnp.float32), None

    summed, _ = lax.scan(block_sum, jnp.zeros((TOKENS, D), jnp.float32), jnp.arange(N_TP, dtype=jnp.int32))
    input_grad = summed.astype(jnp.bfloat16)
    gate_grad = jnp.dot(inputs.T, gate_cot, preferred_element_type=jnp.float32)
    up_grad = jnp.dot(inputs.T, up_cot, preferred_element_type=jnp.float32)
    down_grad = jnp.dot(cotangent.T, hidden, preferred_element_type=jnp.float32) * down_scale
    return (input_grad, gate_grad, up_grad, down_grad)
```

```python
import jax
import jax.numpy as jnp
from jax import lax
from jax.sharding import PartitionSpec as P

BF = jnp.bfloat16
F32 = jnp.float32


def add(*terms):
    total = terms[0].astype(F32)
    for term in terms[1:]:
        total = total + term.astype(F32)
    return total.astype(BF)


def ring_gather(v, n, send):
    rows = v.shape[0]
    out = [(0, 0, v)]
    if n == 1:
        return out
    if n == 2:
        return out + [(1, 0, send(v, 1))]
    fwd, back = v, v
    far = n // 2
    for k in range(1, n - far):
        fwd, back = send(fwd, 1), send(back, -1)
        out += [(k, 0, fwd), (n - k, 0, back)]
    if n % 2 == 0:
        mid = rows // 2
        out += [(far, 0, send(fwd[:mid], 1)), (far, mid, send(back[mid:], -1))]
    return out


def ring_reduce(get, n, send, rows):
    if n == 1:
        return [(0, rows, get(0, 0, rows))]
    if n == 2:
        return [(0, rows, add(get(0, 0, rows), send(get(1, 0, rows), 1)))]

    def chain(sign, count, lo, hi):
        acc = None
        for k in range(count, 0, -1):
            mine = get(sign * k % n, lo, hi)
            acc = send(mine if acc is None else add(mine, acc), sign)
        return acc

    far, near, mid = n // 2, n - 1 - n // 2, rows // 2
    a, b = chain(1, far, 0, mid), chain(-1, far, mid, rows)
    c, d = chain(-1, near, 0, mid), chain(1, near, mid, rows)
    return [(0, mid, add(get(0, 0, mid), a, c)), (mid, rows, add(get(0, mid, rows), b, d))]


def local(
    inputs,
    cotangent,
    gate_pre,
    up_pre,
    gate_weight,
    up_weight,
    down_weight,
    gate_scale,
    up_scale,
    down_scale,
):
    n_fs, n_rep, n_tp = lax.axis_size("fs"), lax.axis_size("rep"), lax.axis_size("tp")
    assert n_rep == 2
    ny = 1
    while (2 * ny) * (2 * ny) <= n_fs and n_fs % (2 * ny) == 0:
        ny *= 2
    nz = n_fs // ny
    rep, fs, tp = lax.axis_index("rep"), lax.axis_index("fs"), lax.axis_index("tp")
    zi, yi = fs // ny, fs % ny
    tokens, width = inputs.shape
    cols = gate_pre.shape[1]
    half = cols // 2
    rows = width // n_fs
    lanes = 128
    c1 = max(half * 5 // 11 // lanes, 1) * lanes
    c2 = half - c1

    def send_z(v, s):
        return lax.ppermute(
            v, "fs", [(z * ny + y, (z + s) % nz * ny + y) for z in range(nz) for y in range(ny)]
        )

    def send_y(v, s):
        return lax.ppermute(
            v, "fs", [(z * ny + y, z * ny + (y + s) % ny) for z in range(nz) for y in range(ny)]
        )

    def swap_x(v):
        return lax.ppermute(v, "rep", [(0, 1), (1, 0)])

    def swap_tp(v):
        return lax.ppermute(v, "tp", [(0, 1), (1, 0)])

    def mine(v):
        return lax.dynamic_slice_in_dim(v, rep * half, half, 1)

    def other(v):
        return lax.dynamic_slice_in_dim(v, (1 - rep) * half, half, 1)

    def with_partner(v):
        part = tokens // n_tp
        got = swap_x(lax.dynamic_slice_in_dim(v, tp * part, part, 0))
        if n_tp == 2:
            also = swap_tp(got)
            first = jnp.where(tp == 0, got, also)
            last = jnp.where(tp == 0, also, got)
            return jnp.concatenate([v, first, last], axis=0)
        return jnp.concatenate([v, lax.all_gather(got, "tp", axis=0, tiled=True)], axis=0)

    def gather(first, second):
        w1, w2 = first.shape[1], second.shape[1]
        out = jnp.zeros((width, w1 + w2), BF)

        def place(out, kz, ky, row, piece, col):
            at = ((zi - kz) % nz * ny + (yi - ky) % ny) * rows + row
            return lax.dynamic_update_slice(out, piece, (at, jnp.int32(col)))

        for kz, row, piece in ring_gather(first, nz, send_z):
            for ky, row2, piece2 in ring_gather(piece, ny, send_y):
                out = place(out, kz, ky, row + row2, piece2, 0)
        for ky, row, piece in ring_gather(second, ny, send_y):
            for kz, row2, piece2 in ring_gather(piece, nz, send_z):
                out = place(out, kz, ky, row + row2, piece2, w1)
        return out

    def reduce(total, w1):
        w2 = total.shape[1] - w1

        def part(kz, ky, lo, hi, col, wide):
            at = ((zi + kz) % nz * ny + (yi + ky) % ny) * rows + lo
            return lax.dynamic_slice(total, (at, jnp.int32(col)), (hi - lo, wide))

        sums = {}

        def y_sum(kz, lo, hi):
            if kz not in sums:
                sums[kz] = ring_reduce(lambda ky, a, b: part(kz, ky, a, b, 0, w1), ny, send_y, rows)
            got = jnp.concatenate([p for _, _, p in sums[kz]], axis=0)
            return got[lo:hi]

        first = ring_reduce(y_sum, nz, send_z, rows)

        zs = {}

        def z_sum(ky, lo, hi):
            if ky not in zs:
                zs[ky] = ring_reduce(lambda kz, a, b: part(kz, ky, a, b, w1, w2), nz, send_z, rows)
            got = jnp.concatenate([p for _, _, p in zs[ky]], axis=0)
            return got[lo:hi]

        second = ring_reduce(z_sum, ny, send_y, rows)
        return [jnp.concatenate([p for _, _, p in s], axis=0) for s in (first, second)]

    def both_halves(v):
        got = swap_x(v)
        return jnp.where(rep == 0, v, got), jnp.where(rep == 0, got, v)

    cot = with_partner(cotangent)
    down = mine(down_weight).astype(BF)
    down_all = gather(down[:, :c1], down[:, c1:])
    gate = jnp.concatenate([mine(gate_pre), swap_x(other(gate_pre))], axis=0).astype(F32)
    upper = jnp.concatenate([mine(up_pre), swap_x(other(up_pre))], axis=0).astype(F32)
    xs = with_partner(inputs)

    gate_w, up_w = mine(gate_weight).astype(BF), mine(up_weight).astype(BF)
    rows_all = gather(
        jnp.concatenate([gate_w[:, :c1], up_w[:, :c1]], axis=1),
        jnp.concatenate([gate_w[:, c1:], up_w[:, c1:]], axis=1),
    )

    sig = jax.nn.sigmoid(gate)
    act = gate * sig
    hidden = (act * upper).astype(BF)
    dims = (((0,), (0,)), ((), ()))
    d_part = lax.dot_general(cot, hidden, dims, preferred_element_type=F32).astype(BF)
    d1, d2 = reduce(d_part, c1)

    hidden_cot = jnp.dot(cot, down_all, preferred_element_type=F32) * mine(down_scale)
    gate_cot = (hidden_cot * upper * sig * (1.0 + gate * (1.0 - sig)) * mine(gate_scale)).astype(BF)
    up_cot = (hidden_cot * act * mine(up_scale)).astype(BF)
    both = jnp.concatenate(
        [gate_cot[:, :c1], up_cot[:, :c1], gate_cot[:, c1:], up_cot[:, c1:]], axis=1
    )
    gu_part = lax.dot_general(xs, both, dims, preferred_element_type=F32).astype(BF)
    gu1, gu2 = reduce(gu_part, 2 * c1)

    partial_value = lax.dot_general(
        both, rows_all, (((1,), (1,)), ((), ())), preferred_element_type=F32
    ).astype(BF)
    if n_tp == 2:
        wide = width // 2
        kept = lax.dynamic_slice_in_dim(partial_value, tp * wide, wide, 1)
        gone = lax.dynamic_slice_in_dim(partial_value, (1 - tp) * wide, wide, 1)
        token_sum = add(kept, swap_tp(gone))
    else:
        token_sum = lax.psum_scatter(partial_value, "tp", scatter_dimension=1, tiled=True)
    input_grad = add(token_sum[:tokens], swap_x(token_sum[tokens:]))

    d1a, d1b = both_halves(d1)
    d2a, d2b = both_halves(d2)
    gu1a, gu1b = both_halves(gu1)
    gu2a, gu2b = both_halves(gu2)
    down_grad = jnp.concatenate([d1a, d2a, d1b, d2b], axis=1).astype(F32) * down_scale
    gate_grad = jnp.concatenate(
        [gu1a[:, :c1], gu2a[:, :c2], gu1b[:, :c1], gu2b[:, :c2]], axis=1
    ).astype(F32)
    up_grad = jnp.concatenate(
        [gu1a[:, c1:], gu2a[:, c2:], gu1b[:, c1:], gu2b[:, c2:]], axis=1
    ).astype(F32)
    return (input_grad, gate_grad, up_grad, down_grad)


def solution(mesh):
    return jax.shard_map(
        local,
        mesh=mesh,
        in_specs=(
            P(("rep", "fs"), None),
            P(("rep", "fs"), None),
            P(("rep", "fs"), "tp"),
            P(("rep", "fs"), "tp"),
            P("fs", "tp"),
            P("fs", "tp"),
            P("fs", "tp"),
            P(None, "tp"),
            P(None, "tp"),
            P(None, "tp"),
        ),
        out_specs=(P(("rep", "fs"), "tp"), P("fs", "tp"), P("fs", "tp"), P("fs", "tp")),
        check_vma=False,
    )
```
